256 devices in a mesh: grp: 2 (over y), ep: 64 (over z, x), tp: 2 (over core).
Axes of the slice: x: 4, y: 2, z: 16, core: 2. Of those that a mesh axis runs over, the one named last changes fastest.
The devices are a block of a 4x16x16 slice.
Arguments:
- tokens: bfloat16 [2048, 1024], P(('grp', 'ep')), parts along dimension 0, may hold values from -6 to 6
- query_weight: bfloat16 [1024, 512], P(None, 'tp'), may hold values from -0.1875 to 0.1875
- key_weight: bfloat16 [1024, 512], P(None, 'tp'), may hold values from -0.1875 to 0.1875
- value_weight: bfloat16 [1024, 512], P(None, 'tp'), may hold values from -0.1875 to 0.1875
- outgate_weight: bfloat16 [1024, 512], P(None, 'tp'), may hold values from -0.1875 to 0.1875
- ingate_weight: bfloat16 [1024, 4], P(None, 'tp'), may hold values from -0.1875 to 0.1875
- forget_weight: bfloat16 [1024, 4], P(None, 'tp'), may hold values from -0.1875 to 0.1875
- forget_bias: float32 [4], P('tp'), may hold values from -2 to 5
- head_gain: float32 [4, 128], P('tp'), may hold values from 0.1 to 1.9
- merge_weight: bfloat16 [512, 1024], P('tp'), may hold values from -0.25 to 0.25
- mixer_gain: float32 [1024], replicated, may hold values from 0.1 to 1.9
- feed_gain: float32 [1024], replicated, may hold values from 0.1 to 1.9
- memory_matrix: float32 [2048, 4, 128, 128], P(('grp', 'ep'), 'tp'), parts along dimension 0, may hold values from -0.6 to 0.6
- memory_norm: float32 [2048, 4, 128], P(('grp', 'ep'), 'tp'), parts along dimension 0, may hold values from -0.6 to 0.6
- memory_max: float32 [2048, 4], P(('grp', 'ep'), 'tp'), parts along dimension 0, may hold values from -4 to 4
- routes: int32 [2048, 2], P(('grp', 'ep')), parts along dimension 0, may hold values from 0 to 63, all different within a row; in each aligned block of 16 rows (0 to 15, 16 to 31, ...) at most 2 rows name the same one
- route_scores: bfloat16 [2048, 2], P(('grp', 'ep')), parts along dimension 0, may hold values from -4 to 4
- expert_gate: bfloat16 [64, 1024, 1792], P('ep', None, 'tp'), may hold values from -0.1875 to 0.1875
- expert_up: bfloat16 [64, 1024, 1792], P('ep', None, 'tp'), may hold values from -0.1875 to 0.1875
- expert_down: bfloat16 [64, 1792, 1024], P('ep', 'tp'), may hold values from -0.125 to 0.125
- dense_left: bfloat16 [1024, 2816], P(None, 'ep'), may hold values from -0.1875 to 0.1875
- dense_right: bfloat16 [1024, 2816], P(None, 'ep'), may hold values from -0.1875 to 0.1875
- dense_down: bfloat16 [2816, 1024], P('ep'), may hold values from -0.109375 to 0.109375
- blend_weight: float32 [1024], replicated, may hold values from -0.1875 to 0.1875
Outputs:
- layer_out: bfloat16 [2048, 1024], P(('grp', 'ep', 'tp')), parts along dimension 0
- new_matrix: float32 [2048, 4, 128, 128], P(('grp', 'ep'), 'tp'), parts along dimension 0
- new_norm: float32 [2048, 4, 128], P(('grp', 'ep'), 'tp'), parts along dimension 0
- new_max: float32 [2048, 4], P(('grp', 'ep'), 'tp'), parts along dimension 0
The draws below stay inside these ranges and needn't reach their ends.
There are 2 independent parts, one for each index of `grp`. The reference program is written for one: setup_inputs(seed, part) draws one part's arguments, and reference() takes and returns one part's arrays. A program takes and returns all parts, laid end to end along the dimension named above; an argument that names none is the same for every part. Nothing has to cross between parts.
Inputs may be any that keep to these rules, and one draw needn't show every extreme that they name: `routes`: each row names 2 different experts. Among the rows of one device (aligned blocks of 16 rows) no expert is named more than 2 times, and in every draw some expert is named exactly 2 times in some block.
All inputs are finite; a program needn't handle non-finite values.
Results may differ from the reference program's by a relative error of at most 0.014.
Values may be sent and summed in bfloat16 or wider, within the bound.
A program may use at most 64 MiB of HBM per device.

```python
import math
import jax
import jax.numpy as jnp
import numpy as np
from jax import lax

D = 1024
HEADS = 4
DH = 128
MW = 512
FFE = 1792
FFD = 2816
TOP = 2
SEQ_DEV = 16
EXPERTS = 64
TOKENS = 1024
CAP = 2
N_EP = 64
N_TP = 2


def block_scale(key, dims, split, low, largest):
    factor_of, own = 1.0, jax.random.fold_in(key, 6)
    for axis_at, blocks in split:
        heights = jnp.exp(jax.random.uniform(jax.random.fold_in(own, axis_at), (blocks,), jnp.float32, low / len(split), largest / len(split)))
        factor_of = factor_of * jnp.repeat(heights, dims[axis_at] // blocks).reshape([-1 if axis == axis_at else 1 for axis in range(len(dims))])
    return factor_of


def deal_out(own_key, own, number, rows, amount, top, limit, skew):
    sequence = jax.random.permutation(own_key, amount)
    packed, ordinary = portions_of(amount, rows * top, limit, skew, True), portions_of(amount, rows * top, limit, skew, False)
    places = jnp.arange(amount)

    def named(tallies, turn):
        used = int((tallies > 0).sum())
        fixed = max(1, used // 4)
        moved = fixed + (places - fixed + turn * (used - fixed)) % max(1, amount - fixed)
        return jnp.zeros((amount,), jnp.int32).at[sequence[jnp.where(places < fixed, places, moved)]].set(jnp.asarray(tallies, jnp.int32))

    tallies = jnp.where(number % 4 == 0, named(packed, number // 4), named(ordinary, number - number // 4 - 1))
    mixed = jax.random.permutation(jax.random.fold_in(own, 3), amount)
    giver, taker = mixed[0:amount // 2 * 2:2], mixed[1:amount // 2 * 2:2]
    room = jnp.minimum(tallies[giver] - 1, limit - tallies[taker]) // 2
    room = jnp.where((giver == sequence[0]) | (taker == sequence[0]) | (tallies[taker] == 0), 0, jnp.maximum(room, 0))
    moved = jax.random.randint(jax.random.fold_in(own, 4), (amount // 2,), 0, 1 << 20) % (room + 1)
    tallies = tallies.at[giver].add(-moved).at[taker].add(moved)
    members = jnp.searchsorted(jnp.cumsum(tallies), jnp.arange(rows * top), side="right").astype(jnp.int32)
    table = members.reshape(top, rows).T
    table = table[jax.random.permutation(jax.random.fold_in(own, 1), rows)]
    turn = jax.random.randint(jax.random.fold_in(own, 2), (rows, 1), 0, top)
    return jnp.take_along_axis(table, (jnp.arange(top)[None, :] + turn) % top, axis=1)


def portions_of(amount, total, reach, skew, full):
    weights = [(1 << 20) // math.isqrt(standing ** skew) + 1 for standing in range(1, amount + 1)]
    largest = reach if full else min(reach, max(-(-total // amount), total * weights[0] // sum(weights)))
    least = 1 if total - largest >= amount - 1 else 0
    given, rest = [largest] + [least] * (amount - 1), total - largest - least * (amount - 1)
    while rest > 0:
        movable = [i for i in range(1, amount) if given[i] < largest] or [i for i in range(1, amount) if given[i] < reach]
        mass, left = sum([weights[i] for i in movable]), rest
        for i in movable:
            more = min(reach - given[i], max(1, left * weights[i] // mass), rest)
            given[i] = given[i] + more
            rest = rest - more
    return np.array(given)


def centred(own_key, dims, spread, limit, pieces=(), kind=jnp.bfloat16):
    entries = jax.random.normal(own_key, dims, jnp.float32) * spread
    if len(pieces) > 0:
        entries = block_scale(own_key, dims, pieces, -0.22, 0.18) * entries
    return jnp.clip(entries, min=-limit, max=limit).astype(kind)


def setup_inputs(seed: int = 0, part: int = 0) -> dict:
    splits = jax.random.split(jax.random.key(seed), 25)
    own_keys = jax.random.split(jax.random.fold_in(splits[24], part), 25)
    tokens = centred(own_keys[0], (TOKENS, D), 1.0, 6.0, ((0, 64),))
    query_weight = centred(splits[1], (D, MW), D ** -0.5, 0.1875, ((1, 2),))
    key_weight = centred(splits[2], (D, MW), D ** -0.5, 0.1875, ((1, 2),))
    value_weight = centred(splits[3], (D, MW), D ** -0.5, 0.1875, ((1, 2),))
    outgate_weight = centred(splits[4], (D, MW), D ** -0.5, 0.1875, ((1, 2),))
    ingate_weight = centred(splits[5], (D, HEADS), D ** -0.5, 0.1875, ((1, 2),))
    forget_weight = centred(splits[6], (D, HEADS), D ** -0.5, 0.1875, ((1, 2),))
    forget_bias = jnp.clip(-2.0 + 7.0 * jax.random.uniform(splits[7], (HEADS,), jnp.float32) ** block_scale(splits[7], (HEADS,), ((0, 2),), -0.2, 0.2), -2.0, 5.0)
    head_gain = jnp.clip(1.0 + 0.18 * jax.random.normal(splits[8], (HEADS, DH), jnp.float32), 0.1, 1.9)
    merge_weight = centred(splits[9], (MW, D), MW ** -0.5, 0.25, ((0, 2),))
    mixer_gain = jnp.clip(1.0 + 0.18 * jax.random.normal(splits[10], (D,), jnp.float32), 0.1, 1.9)
    feed_gain = jnp.clip(1.0 + 0.18 * jax.random.normal(splits[11], (D,), jnp.float32), 0.1, 1.9)
    memory_matrix = centred(own_keys[12], (TOKENS, HEADS, DH, DH), 0.1, 0.6, ((0, 64), (1, 2)), jnp.float32)
    memory_norm = centred(own_keys[13], (TOKENS, HEADS, DH), 0.1, 0.6, ((0, 64), (1, 2)), jnp.float32)
    memory_max = centred(own_keys[14], (TOKENS, HEADS), 1.0, 4.0, ((0, 64), (1, 2)), jnp.float32)
    routes_keys = jax.random.split(jax.random.fold_in(own_keys[15], 1), TOKENS // SEQ_DEV)
    routes_turns = jax.random.permutation(jax.random.fold_in(own_keys[15], 3), TOKENS // SEQ_DEV)
    routes = jax.vmap(lambda own, number: deal_out(jax.random.fold_in(own_keys[15], 2), own, number, SEQ_DEV, EXPERTS, TOP, CAP, 2))(routes_keys, routes_turns).reshape((TOKENS, TOP))
    route_scores = centred(own_keys[16], (TOKENS, TOP), 1.0, 4.0, ((0, 64),))
    expert_gate = centred(splits[17], (EXPERTS, D, FFE), D ** -0.5, 0.1875, ((0, 64), (2, 2)))
    expert_up = centred(splits[18], (EXPERTS, D, FFE), D ** -0.5, 0.1875, ((0, 64), (2, 2)))
    expert_down = centred(splits[19], (EXPERTS, FFE, D), FFE ** -0.5, 0.125, ((0, 64), (1, 2)))
    dense_left = centred(splits[20], (D, FFD), D ** -0.5, 0.1875, ((1, 64),))
    dense_right = centred(splits[21], (D, FFD), D ** -0.5, 0.1875, ((1, 64),))
    dense_down = centred(splits[22], (FFD, D), FFD ** -0.5, 0.109375, ((0, 64),))
    blend_weight = centred(splits[23], (D,), D ** -0.5, 0.1875, (), jnp.float32)
    return {"tokens": tokens, "query_weight": query_weight, "key_weight": key_weight, "value_weight": value_weight, "outgate_weight": outgate_weight, "ingate_weight": ingate_weight, "forget_weight": forget_weight, "forget_bias": forget_bias, "head_gain": head_gain, "merge_weight": merge_weight, "mixer_gain": mixer_gain, "feed_gain": feed_gain, "memory_matrix": memory_matrix, "memory_norm": memory_norm, "memory_max": memory_max, "routes": routes, "route_scores": route_scores, "expert_gate": expert_gate, "expert_up": expert_up, "expert_down": expert_down, "dense_left": dense_left, "dense_right": dense_right, "dense_down": dense_down, "blend_weight": blend_weight}


epsilon = 1e-06

def rms_norm(values, gains):
    floats = values.astype(jnp.float32)
    scaled = floats * lax.rsqrt(lax.optimization_barrier(jnp.mean(floats * floats, axis=-1, keepdims=True)) + epsilon)
    return (scaled * gains).astype(jnp.bfloat16)

def memory_step(query_rows, key_rows, value_rows, in_gate, forget_pre, matrix, norm_vec, old_max):
    log_forget = jax.nn.log_sigmoid(forget_pre)
    new_max = jnp.maximum(log_forget + old_max, in_gate)
    keep = jnp.exp(log_forget + old_max - new_max)
    write = jnp.exp(in_gate - new_max)
    matrix = keep[..., None, None] * matrix + write[..., None, None] * key_rows[..., :, None] * value_rows[..., None, :]
    norm_vec = keep[..., None] * norm_vec + write[..., None] * key_rows
    numer = jnp.einsum('bhd,bhde->bhe', query_rows, matrix, precision=lax.Precision.HIGHEST)
    denom = lax.optimization_barrier(jnp.sum(query_rows * norm_vec, axis=-1))
    readout = numer / jnp.maximum(jnp.abs(denom), jnp.exp(-new_max))[..., None]
    return (readout, matrix, norm_vec, new_max)

def halves_sum(hidden, down, parts):
    width = hidden.shape[1] // parts
    total = jnp.zeros((hidden.shape[0], down.shape[1]), jnp.float32)
    for index in range(parts):
        piece = jnp.dot(hidden[:, index * width:(index + 1) * width], down[index * width:(index + 1) * width], preferred_element_type=jnp.float32).astype(jnp.bfloat16)
        piece = lax.optimization_barrier(piece)
        total = total + piece.astype(jnp.float32)
    return total

def reference(tokens, query_weight, key_weight, value_weight, outgate_weight, ingate_weight, forget_weight, forget_bias, head_gain, merge_weight, mixer_gain, feed_gain, memory_matrix, memory_norm, memory_max, routes, route_scores, expert_gate, expert_up, expert_down, dense_left, dense_right, dense_down, blend_weight):
    rows_all = tokens.shape[0]
    normed = rms_norm(tokens, mixer_gain)

    def project(weight):
        return jnp.dot(normed, weight, preferred_element_type=jnp.float32)
    query = project(query_weight).reshape(rows_all, HEADS, DH)
    key_rows = project(key_weight).reshape(rows_all, HEADS, DH) * DH ** (-0.5)
    value_rows = project(value_weight).reshape(rows_all, HEADS, DH)
    outgate_rows = project(outgate_weight).reshape(rows_all, HEADS, DH)
    in_gate = project(ingate_weight)
    forget_pre = project(forget_weight) + forget_bias
    readout, matrix, norm_vec, new_max = memory_step(query, key_rows, value_rows, in_gate, forget_pre, memory_matrix, memory_norm, memory_max)
    head_scale = lax.rsqrt(lax.optimization_barrier(jnp.mean(readout * readout, axis=(1, 2))) + epsilon)
    gated = (readout * head_gain * jax.nn.sigmoid(outgate_rows)).reshape(rows_all, MW).astype(jnp.bfloat16)
    head_total = jnp.dot(gated, merge_weight, preferred_element_type=jnp.float32)
    resid = (tokens.astype(jnp.float32) + head_scale[:, None] * head_total).astype(jnp.bfloat16)
    normed2 = rms_norm(resid, feed_gain)
    assign = SEQ_DEV * TOP
    routes_block = routes.reshape(N_EP, assign)
    member = (routes_block[..., None] == jnp.arange(EXPERTS, dtype=jnp.int32)).astype(jnp.int32)
    slot_rank = lax.optimization_barrier(jnp.sum(member * (jnp.cumsum(member, axis=1) - member), axis=-1)).astype(jnp.int32)
    source_ids = jnp.broadcast_to(jnp.arange(N_EP, dtype=jnp.int32)[:, None], (N_EP, assign))
    spread_rows = jnp.repeat(normed2, TOP, axis=0).reshape(N_EP, assign, D)
    inbox = jnp.zeros((EXPERTS, N_EP, CAP, D), jnp.bfloat16).at[routes_block, source_ids, slot_rank].set(spread_rows)

    def run_expert(operands):
        box, gate_w, up_w, down_w = operands
        rows = box.reshape(N_EP * CAP, D)
        gate_val = jnp.dot(rows, gate_w, preferred_element_type=jnp.float32)
        up_val = jnp.dot(rows, up_w, preferred_element_type=jnp.float32)
        hidden = (jax.nn.silu(gate_val) * up_val).astype(jnp.bfloat16)
        total = halves_sum(hidden, down_w, N_TP)
        return total.astype(jnp.bfloat16).reshape(N_EP, CAP, D)
    outbox = lax.map(run_expert, (inbox, expert_gate, expert_up, expert_down))
    picked = outbox[routes_block, source_ids, slot_rank].reshape(rows_all, TOP, D).astype(jnp.float32)
    route_weight = jax.nn.softmax(route_scores.astype(jnp.float32), axis=-1)
    routed = lax.optimization_barrier(jnp.sum(route_weight[..., None] * picked, axis=1))
    left_val = jnp.dot(normed2, dense_left, preferred_element_type=jnp.float32)
    right_val = jnp.dot(normed2, dense_right, preferred_element_type=jnp.float32)
    dense_hidden = (jax.nn.silu(left_val) * right_val).astype(jnp.bfloat16)
    dense = jnp.dot(dense_hidden, dense_down, preferred_element_type=jnp.float32)
    blend = jax.nn.sigmoid(lax.optimization_barrier(jnp.sum(normed2.astype(jnp.float32) * blend_weight, axis=-1)))
    layer_out = (resid.astype(jnp.float32) + routed + blend[:, None] * dense).astype(jnp.bfloat16)
    return (layer_out, matrix, norm_vec, new_max)
```

```python
import functools

import jax
import jax.numpy as jnp
from jax import lax
from jax.experimental import pallas as pl
from jax.experimental.pallas import tpu as pltpu
from jax.sharding import PartitionSpec as P

MESH = pl.DeviceIdType.MESH
GRP_EP = ("grp", "ep")
GRP_EP_TP = ("grp", "ep", "tp")
NX = 4
SPAN = 2
PADDED = 48
LANES = 128

epsilon = 1e-06


def rms_norm(values, gains):
    floats = values.astype(jnp.float32)
    scaled = floats * lax.rsqrt(jnp.mean(floats * floats, axis=-1, keepdims=True) + epsilon)
    return (scaled * gains).astype(jnp.bfloat16)


def memory_step(query_rows, key_rows, value_rows, in_gate, forget_pre, matrix, norm_vec, old_max):
    log_forget = jax.nn.log_sigmoid(forget_pre)
    new_max = jnp.maximum(log_forget + old_max, in_gate)
    keep = jnp.exp(log_forget + old_max - new_max)
    write = jnp.exp(in_gate - new_max)
    matrix = (
        keep[..., None, None] * matrix
        + write[..., None, None] * key_rows[..., :, None] * value_rows[..., None, :]
    )
    norm_vec = keep[..., None] * norm_vec + write[..., None] * key_rows
    numer = jnp.einsum("bhd,bhde->bhe", query_rows, matrix, precision=lax.Precision.HIGHEST)
    denom = jnp.sum(query_rows * norm_vec, axis=-1)
    readout = numer / jnp.maximum(jnp.abs(denom), jnp.exp(-new_max))[..., None]
    return (readout, matrix, norm_vec, new_max)


def dot32(a, b, precision=None):
    return jnp.dot(a, b, preferred_element_type=jnp.float32, precision=precision)


def dot_nt(a, b):
    return lax.dot_general(a, b, (((1,), (1,)), ((), ())), preferred_element_type=jnp.float32)


def dot_tn(a, b):
    return lax.dot_general(a, b, (((0,), (0,)), ((), ())), preferred_element_type=jnp.float32)


def feed_kernel(
    nep,
    nx,
    span,
    all_width,
    tokens_ref,
    part_ref,
    routes_ref,
    scores_ref,
    gain_ref,
    blend_ref,
    block_ref,
    gate_hbm,
    up_hbm,
    down_hbm,
    out_ref,
    gate_v,
    up_v,
    down_v,
    part_in,
    resid_v,
    normed_v,
    relay,
    outbox,
    inbox,
    rows_v,
    half_out,
    half_in,
    backbox,
    homebox,
    acts_out,
    acts,
    blocks,
    dense_out,
    dense_in,
    swap_out,
    swap_in,
    local_sem,
    send_sem,
    recv_sem,
    block_send,
    block_recv,
):
    t = lax.axis_index("tp")
    me = lax.axis_index("ep")
    z, x = me // nx, me % nx
    nz = nep // nx
    members = nz // span
    own_rows, width = tokens_ref.shape
    half = width // 2
    pieces = half // LANES
    half_rows = own_rows // 2
    zi, zr = z // span, z % span
    my_block = zr * nx + x
    peers = nep - 1
    partner = {"tp": 1 - t}

    def remote(src, dst, send, recv, device):
        return pltpu.make_async_remote_copy(
            src_ref=src, dst_ref=dst, send_sem=send, recv_sem=recv, device_id=device, device_id_type=MESH
        )

    def await_bytes(ref, sem):
        pltpu.make_async_copy(ref, ref, sem).wait()

    barrier = pltpu.get_barrier_semaphore()

    @pl.loop(1, nep)
    def _(i):
        pl.semaphore_signal(barrier, inc=1, device_id={"ep": (me + i) % nep}, device_id_type=MESH)

    pl.semaphore_signal(barrier, inc=1, device_id=partner, device_id_type=MESH)
    loads = [
        pltpu.make_async_copy(src, dst, local_sem.at[i])
        for i, (src, dst) in enumerate(((gate_hbm.at[0], gate_v), (up_hbm.at[0], up_v), (down_hbm.at[0], down_v)))
    ]
    for load in loads:
        load.start()
    blocks[my_block] = block_ref[...]
    mine = pl.ds(pl.multiple_of(t * half, LANES), half)
    pl.semaphore_wait(barrier, nep)

    exchange = remote(part_ref, part_in, send_sem.at[0], recv_sem.at[0], partner)
    exchange.start()

    def block_copy(index, device, slot):
        ref = blocks.at[index, :, mine]
        return remote(ref, ref, block_send.at[slot], block_recv.at[index], device)

    if span == 2:
        pair = block_copy(my_block, {"ep": (z + 1 - 2 * zr) * nx + x}, 0)
        pair.start()
    exchange.wait()

    total = part_ref[...] + part_in[...]
    scale = lax.rsqrt(total[:, width : width + 1] / all_width + epsilon)
    resid = (tokens_ref[...].astype(jnp.float32) + scale * total[:, :width]).astype(jnp.bfloat16)
    resid32 = resid.astype(jnp.float32)
    resid_v[...] = resid32
    normed = rms_norm(resid32, gain_ref[...])
    normed_v[...] = normed.astype(jnp.float32)

    experts = lax.broadcasted_iota(jnp.int32, (own_rows, nep), 1)
    picks = [(routes_ref[:, k : k + 1] == experts).astype(jnp.float32) for k in range(2)]
    member = picks[0] + picks[1]
    row_at = lax.broadcasted_iota(jnp.int32, (own_rows, own_rows), 0)
    col_at = lax.broadcasted_iota(jnp.int32, (own_rows, own_rows), 1)
    earlier = (col_at < row_at).astype(jnp.float32)
    rank = dot32(earlier, member)
    chosen = [jnp.where(rank < 0.5, member, 0.0), jnp.where(rank < 0.5, 0.0, member)]

    def to_boxes(values, box):
        for slot in range(2):
            for c in range(pieces):
                relay[pl.ds(slot * pieces + c, nep, stride=2 * pieces), :] = values[slot][
                    :, c * LANES : (c + 1) * LANES
                ]
        box[...] = relay[...].reshape(nep, 2 * pieces, LANES).astype(jnp.bfloat16)

    def from_box(box, slot, c):
        return relay[pl.ds(slot * pieces + c, nep, stride=2 * pieces), :]

    own_half = normed_v[:, mine].astype(jnp.bfloat16)
    to_boxes([dot_tn(chosen[s].astype(jnp.bfloat16), own_half) for s in range(2)], outbox)

    def send_all(src, dst_at, sem):
        @pl.loop(0, nz)
        def _(k):
            away = nz // 2 + (2 * (k % 2) - 1) * ((k + 1) // 2)
            there_z = (z + away) % nz
            for j in range(nx):
                there = there_z * nx + (x + j) % nx

                @pl.when(there != me)
                def _():
                    remote(src.at[there], dst_at, send_sem.at[sem], recv_sem.at[sem], {"ep": there}).start()

    send_all(outbox, inbox.at[t, me], 1)
    inbox[t, me] = outbox[me]

    acts_out[...] = normed_v[pl.ds(pl.multiple_of(t * half_rows, half_rows), half_rows), :].astype(jnp.bfloat16)

    def block_to_x(index, base):
        copies = [block_copy(index, {"ep": z * nx + (x + j) % nx}, base + j) for j in range(1, nx)]
        for copy in copies:
            copy.start()
        return copies

    sent = block_to_x(my_block, 0)

    @pl.loop(1, members)
    def _(i):
        there = ((zi + i) % members) * span + zr
        remote(acts_out, acts.at[zi], send_sem.at[2], recv_sem.at[2], {"ep": there * nx + x}).start()

    acts[zi] = acts_out[...]

    def await_block(index):
        ref = blocks.at[index, :, mine]
        pltpu.make_async_copy(ref, ref, block_recv.at[index]).wait()

    if span == 2:
        other = (1 - zr) * nx + x
        await_block(other)
        sent += block_to_x(other, nx)

    box_bytes = inbox.at[0, pl.ds(0, peers)]
    await_bytes(box_bytes, recv_sem.at[1])
    box_swap = remote(inbox.at[t], inbox.at[t], send_sem.at[3], recv_sem.at[3], partner)
    box_swap.start()
    box_swap.wait_recv()

    for h in range(2):
        relay[...] = inbox[h].astype(jnp.float32).reshape(relay.shape)
        for slot in range(2):
            for c in range(pieces):
                at = h * half + c * LANES
                rows_v[slot * nep : (slot + 1) * nep, at : at + LANES] = from_box(relay, slot, c).astype(jnp.bfloat16)
    loads[0].wait()
    loads[1].wait()
    gate_val = dot32(rows_v[...], gate_v[...])
    up_val = dot32(rows_v[...], up_v[...])
    hidden = (jax.nn.silu(gate_val) * up_val).astype(jnp.bfloat16)
    loads[2].wait()
    for h in range(2):
        half_out[h] = dot32(hidden, down_v[:, h * half : (h + 1) * half]).astype(jnp.bfloat16)
    half_swap = remote(half_out.at[1 - t], half_in, send_sem.at[4], recv_sem.at[4], partner)
    half_swap.start()

    theirs = pl.ds(pl.multiple_of((1 - t) * half, LANES), half)

    def block_swap(index):
        ref = blocks.at[index, :, mine]
        return remote(ref, ref, block_send.at[2 * nx + index], block_recv.at[span * nx + index], partner)

    for i in range(1, span * nx):
        index = (my_block + i) % (span * nx)
        if not (span == 2 and i == nx):
            await_block(index)
        block_swap(index).start()

    half_swap.wait_recv()
    summed = (half_out[t].astype(jnp.float32) + half_in[...].astype(jnp.float32)).astype(jnp.bfloat16)
    summed = summed.astype(jnp.float32)
    await_bytes(box_bytes, send_sem.at[1])
    to_boxes([summed[s * nep : (s + 1) * nep] for s in range(2)], backbox)
    send_all(backbox, homebox.at[me], 5)
    homebox[me] = backbox[me]

    for i in range(1, span * nx):
        index = (my_block + i) % (span * nx)
        ref = blocks.at[index, :, theirs]
        pltpu.make_async_copy(ref, ref, block_recv.at[span * nx + index]).wait()
    act_bytes = acts.at[pl.ds(0, members - 1)]
    await_bytes(act_bytes, recv_sem.at[2])
    dense_rows = acts[...].astype(jnp.float32).reshape(members * half_rows, width).astype(jnp.bfloat16)
    dense = jnp.zeros((members * half_rows, width), jnp.float32)
    for index in range(span * nx):
        left = dot_nt(dense_rows, blocks[index, 0:PADDED, :])
        right = dot_nt(dense_rows, blocks[index, PADDED : 2 * PADDED, :])
        units = (jax.nn.silu(left) * right).astype(jnp.bfloat16)
        dense = dense + dot32(units, blocks[index, 2 * PADDED : 3 * PADDED, :])
    dense_out[...] = dense.reshape(members, half_rows, width).astype(jnp.bfloat16)

    @pl.loop(1, members)
    def _(i):
        mi = (zi + i) % members
        there = mi * span + zr
        remote(dense_out.at[mi], dense_in.at[zi], send_sem.at[6], recv_sem.at[6], {"ep": there * nx + x}).start()

    dense_in[zi] = dense_out[zi]

    scores = scores_ref[...].astype(jnp.float32)
    top = jnp.max(scores, axis=-1, keepdims=True)
    powers = jnp.exp(scores - top)
    weights = powers / jnp.sum(powers, axis=-1, keepdims=True)
    weight_of = weights[:, 0:1] * picks[0] + weights[:, 1:2] * picks[1]
    await_bytes(homebox.at[pl.ds(0, peers)], recv_sem.at[5])
    relay[...] = homebox[...].astype(jnp.float32).reshape(relay.shape)
    routed = []
    for c in range(pieces):
        piece = jnp.zeros((own_rows, LANES), jnp.float32)
        for slot in range(2):
            taken = jnp.where(chosen[slot] > 0.5, weight_of, 0.0)
            piece = piece + dot32(taken, from_box(relay, slot, c), lax.Precision.HIGHEST)
        routed.append(piece)
    routed = jnp.concatenate(routed, axis=1)
    for h in range(2):
        swap_out[h] = routed[h * half_rows : (h + 1) * half_rows]
    swap = remote(swap_out.at[1 - t], swap_in, send_sem.at[7], recv_sem.at[7], partner)
    swap.start()

    home = pl.ds(pl.multiple_of(t * half_rows, half_rows), half_rows)
    own_normed = normed_v[home, :]
    blend = jax.nn.sigmoid(jnp.sum(own_normed * blend_ref[...], axis=-1, keepdims=True))
    await_bytes(dense_in.at[pl.ds(0, members - 1)], recv_sem.at[6])
    base = resid_v[home, :] + blend * jnp.sum(dense_in[...].astype(jnp.float32), axis=0)
    resid_v[home, :] = base
    swap.wait_recv()
    out_ref[:, mine] = (resid_v[home, mine] + swap_out[t]).astype(jnp.bfloat16)
    out_ref[:, theirs] = (resid_v[home, theirs] + swap_in[...]).astype(jnp.bfloat16)

    await_bytes(act_bytes, send_sem.at[2])
    box_swap.wait_send()
    half_swap.wait_send()
    await_bytes(box_bytes, send_sem.at[5])
    await_bytes(dense_in.at[pl.ds(0, members - 1)], send_sem.at[6])
    swap.wait_send()
    if span == 2:
        pair.wait_send()
    for copy in sent:
        copy.wait_send()
    for i in range(1, span * nx):
        block_swap((my_block + i) % (span * nx)).wait_send()


def feed(nep, nx, span, all_width, tokens, part, routes, scores, gain, blend, block, gate, up, down):
    own_rows, width = tokens.shape
    half, half_rows = width // 2, own_rows // 2
    pieces = half // LANES
    members = nep // nx // span
    hidden = gate.shape[2]
    bf16, f32 = jnp.bfloat16, jnp.float32
    vmem = pl.BlockSpec(memory_space=pltpu.VMEM)
    anywhere = pl.BlockSpec(memory_space=pl.ANY)
    box = (nep, 2 * pieces, LANES)
    return pl.pallas_call(
        functools.partial(feed_kernel, nep, nx, span, all_width),
        out_shape=jax.ShapeDtypeStruct((half_rows, width), bf16),
        in_specs=[vmem] * 7 + [anywhere] * 3,
        out_specs=vmem,
        scratch_shapes=[
            pltpu.VMEM((width, hidden), bf16),
            pltpu.VMEM((width, hidden), bf16),
            pltpu.VMEM((hidden, width), bf16),
            pltpu.VMEM((own_rows, width + LANES), f32),
            pltpu.VMEM((own_rows, width), f32),
            pltpu.VMEM((own_rows, width), f32),
            pltpu.VMEM((nep * 2 * pieces, LANES), f32),
            pltpu.VMEM(box, bf16),
            pltpu.VMEM((2, *box), bf16),
            pltpu.VMEM((2 * nep, width), bf16),
            pltpu.VMEM((2, 2 * nep, half), bf16),
            pltpu.VMEM((2 * nep, half), bf16),
            pltpu.VMEM(box, bf16),
            pltpu.VMEM(box, bf16),
            pltpu.VMEM((half_rows, width), bf16),
            pltpu.VMEM((members, half_rows, width), bf16),
            pltpu.VMEM((span * nx, 3 * PADDED, width), bf16),
            pltpu.VMEM((members, half_rows, width), bf16),
            pltpu.VMEM((members, half_rows, width), bf16),
            pltpu.VMEM((2, half_rows, half), f32),
            pltpu.VMEM((half_rows, half), f32),
            pltpu.SemaphoreType.DMA((3,)),
            pltpu.SemaphoreType.DMA((8,)),
            pltpu.SemaphoreType.DMA((8,)),
            pltpu.SemaphoreType.DMA((2 * nx + span * nx,)),
            pltpu.SemaphoreType.DMA((2 * span * nx,)),
        ],
        compiler_params=pltpu.CompilerParams(
            collective_id=0, has_side_effects=True, vmem_limit_bytes=48 * 1024 * 1024
        ),
        name="feed",
    )(tokens, part, routes, scores, gain, blend, block, gate, up, down)


def local(
    nx,
    span,
    tokens,
    query_weight,
    key_weight,
    value_weight,
    outgate_weight,
    ingate_weight,
    forget_weight,
    forget_bias,
    head_gain,
    merge_weight,
    mixer_gain,
    feed_gain,
    memory_matrix,
    memory_norm,
    memory_max,
    routes,
    route_scores,
    expert_gate,
    expert_up,
    expert_down,
    dense_left,
    dense_right,
    dense_down,
    blend_weight,
):
    own_rows = tokens.shape[0]
    heads_here = forget_bias.shape[0]
    head_size = head_gain.shape[1]
    width_here = heads_here * head_size
    normed = rms_norm(tokens, mixer_gain)

    def project(weight):
        return jnp.dot(normed, weight, preferred_element_type=jnp.float32)

    query = project(query_weight).reshape(own_rows, heads_here, head_size)
    key_rows = project(key_weight).reshape(own_rows, heads_here, head_size) * head_size ** (-0.5)
    value_rows = project(value_weight).reshape(own_rows, heads_here, head_size)
    outgate_rows = project(outgate_weight).reshape(own_rows, heads_here, head_size)
    in_gate = project(ingate_weight)
    forget_pre = project(forget_weight) + forget_bias
    readout, matrix, norm_vec, new_max = memory_step(
        query, key_rows, value_rows, in_gate, forget_pre, memory_matrix, memory_norm, memory_max
    )
    energy = jnp.sum(readout * readout, axis=(1, 2))
    gated = (
        (readout * head_gain * jax.nn.sigmoid(outgate_rows))
        .reshape(own_rows, width_here)
        .astype(jnp.bfloat16)
    )
    head_part = jnp.dot(gated, merge_weight, preferred_element_type=jnp.float32)
    part = jnp.concatenate([head_part, jnp.broadcast_to(energy[:, None], (own_rows, LANES))], axis=1)

    def padded(rows):
        return jnp.pad(rows, ((0, PADDED - rows.shape[0]), (0, 0)))

    block = jnp.concatenate([padded(dense_left.T), padded(dense_right.T), padded(dense_down)], axis=0)
    layer_out = feed(
        lax.axis_size("ep"),
        nx,
        span,
        width_here * lax.axis_size("tp"),
        tokens,
        part,
        routes,
        route_scores,
        feed_gain[None, :],
        blend_weight[None, :],
        block,
        expert_gate,
        expert_up,
        expert_down,
    )
    return (layer_out, matrix, norm_vec, new_max)


def build(mesh, nx, span):
    return jax.shard_map(
        functools.partial(local, nx, span),
        mesh=mesh,
        in_specs=(
            P(GRP_EP, None),
            P(None, "tp"),
            P(None, "tp"),
            P(None, "tp"),
            P(None, "tp"),
            P(None, "tp"),
            P(None, "tp"),
            P("tp"),
            P("tp", None),
            P("tp", None),
            P(),
            P(),
            P(GRP_EP, "tp", None, None),
            P(GRP_EP, "tp", None),
            P(GRP_EP, "tp"),
            P(GRP_EP, None),
            P(GRP_EP, None),
            P("ep", None, "tp"),
            P("ep", None, "tp"),
            P("ep", "tp", None),
            P(None, "ep"),
            P(None, "ep"),
            P("ep", None),
            P(),
        ),
        out_specs=(
            P(GRP_EP_TP, None),
            P(GRP_EP, "tp", None, None),
            P(GRP_EP, "tp", None),
            P(GRP_EP, "tp"),
        ),
        check_vma=False,
    )


def solution(mesh):
    return build(mesh, NX, SPAN)
```

```python
import functools

import jax
import jax.numpy as jnp
from jax import lax
from jax.experimental import pallas as pl
from jax.experimental.pallas import tpu as pltpu
from jax.sharding import PartitionSpec as P

MESH = pl.DeviceIdType.MESH
GRP_EP = ("grp", "ep")
GRP_EP_TP = ("grp", "ep", "tp")
NX = 4
SPAN = 2
PADDED = 48
CHUNKS = 4
LANES = 128

epsilon = 1e-06


def rms_norm(values, gains):
    floats = values.astype(jnp.float32)
    scaled = floats * lax.rsqrt(jnp.mean(floats * floats, axis=-1, keepdims=True) + epsilon)
    return (scaled * gains).astype(jnp.bfloat16)


def dot32(a, b, precision=None):
    return jnp.dot(a, b, preferred_element_type=jnp.float32, precision=precision)


def dot_nt(a, b):
    return lax.dot_general(a, b, (((1,), (1,)), ((), ())), preferred_element_type=jnp.float32)


def dot_tn(a, b):
    return lax.dot_general(a, b, (((0,), (0,)), ((), ())), preferred_element_type=jnp.float32)


def feed_kernel(
    nep,
    nx,
    span,
    all_width,
    tokens_ref,
    routes_ref,
    scores_ref,
    mixer_ref,
    gain_ref,
    blend_ref,
    block_ref,
    inforget_ref,
    bias_ref,
    head_gain_ref,
    norm_ref,
    max_ref,
    query_hbm,
    key_hbm,
    value_hbm,
    outgate_hbm,
    merge_hbm,
    matrix_hbm,
    gate_hbm,
    up_hbm,
    down_hbm,
    out_ref,
    new_matrix_hbm,
    new_norm_ref,
    new_max_ref,
    project_v,
    merge_v,
    matrix_v,
    numer_v,
    part_ref,
    gate_v,
    up_v,
    down_v,
    part_in,
    resid_v,
    normed_v,
    relay,
    outbox,
    inbox,
    rows_v,
    half_out,
    half_in,
    backbox,
    homebox,
    acts_out,
    acts,
    blocks,
    dense_out,
    dense_in,
    swap_out,
    swap_in,
    local_sem,
    send_sem,
    recv_sem,
    block_send,
    block_recv,
):
    t = lax.axis_index("tp")
    me = lax.axis_index("ep")
    z, x = me // nx, me % nx
    nz = nep // nx
    members = nz // span
    own_rows, width = tokens_ref.shape
    half = width // 2
    pieces = half // LANES
    half_rows = own_rows // 2
    zi, zr = z // span, z % span
    my_block = zr * nx + x
    peers = nep - 1
    partner = {"tp": 1 - t}

    def remote(src, dst, send, recv, device):
        return pltpu.make_async_remote_copy(
            src_ref=src, dst_ref=dst, send_sem=send, recv_sem=recv, device_id=device, device_id_type=MESH
        )

    def await_bytes(ref, sem):
        pltpu.make_async_copy(ref, ref, sem).wait()

    barrier = pltpu.get_barrier_semaphore()

    @pl.loop(1, nep)
    def _(i):
        pl.semaphore_signal(barrier, inc=1, device_id={"ep": (me + i) % nep}, device_id_type=MESH)

    pl.semaphore_signal(barrier, inc=1, device_id=partner, device_id_type=MESH)
    moves = [(src, project_v.at[i]) for i, src in enumerate((query_hbm, key_hbm, value_hbm, outgate_hbm))]
    chunk = own_rows // CHUNKS
    for c in range(CHUNKS):
        rows = pl.ds(c * chunk, chunk)
        moves.append((matrix_hbm.at[rows], matrix_v.at[rows]))
    moves += [(merge_hbm, merge_v), (gate_hbm.at[0], gate_v), (up_hbm.at[0], up_v), (down_hbm.at[0], down_v)]
    loads = [pltpu.make_async_copy(src, dst, local_sem.at[i]) for i, (src, dst) in enumerate(moves)]
    stores = [
        pltpu.make_async_copy(dst, new_matrix_hbm.at[pl.ds(c * chunk, chunk)], local_sem.at[len(loads) + c])
        for c, (_, dst) in enumerate(moves[4 : 4 + CHUNKS])
    ]
    for load in loads:
        load.start()
    blocks[my_block] = block_ref[...]
    mine = pl.ds(pl.multiple_of(t * half, LANES), half)

    heads, head = head_gain_ref.shape
    first = rms_norm(tokens_ref[...], mixer_ref[...])
    gates = dot32(first, inforget_ref[...])
    in_gate = gates[:, 0:heads]
    log_forget = jax.nn.log_sigmoid(gates[:, heads : 2 * heads] + bias_ref[...])
    old_max = max_ref[...]
    new_max = jnp.maximum(log_forget + old_max, in_gate)
    new_max_ref[...] = new_max
    keep = jnp.exp(log_forget + old_max - new_max)
    write = jnp.exp(in_gate - new_max)
    floor = jnp.exp(-new_max)
    projected = []
    for i in range(4):
        loads[i].wait()
        projected.append(dot32(first, project_v[i]))
    by_head = [[p[:, h * head : (h + 1) * head] for h in range(heads)] for p in projected]
    queries, keys, values, outgates = by_head
    written = [write[:, h : h + 1] * (keys[h] * head ** (-0.5)) for h in range(heads)]
    columns = jnp.concatenate(queries + written, axis=0).T
    norms = []
    for h in range(heads):
        norm = keep[:, h : h + 1] * norm_ref[:, h * head : (h + 1) * head] + written[h]
        new_norm_ref[:, h * head : (h + 1) * head] = norm
        norms.append(norm)
    for b in range(own_rows):
        if b % chunk == 0:
            loads[4 + b // chunk].wait()
        for h in range(heads):
            at = h * own_rows + b
            to = heads * own_rows + at
            fresh = keep[b : b + 1, h : h + 1] * matrix_v[b, h] + columns[:, to : to + 1] * values[h][b : b + 1, :]
            matrix_v[b, h] = fresh
            numer_v[h, b : b + 1, :] = jnp.sum(columns[:, at : at + 1] * fresh, axis=0, keepdims=True)
        if b % chunk == chunk - 1:
            stores[b // chunk].start()
    energy = jnp.zeros((own_rows, 1), jnp.float32)
    gated = []
    for h in range(heads):
        denom = jnp.sum(queries[h] * norms[h], axis=-1, keepdims=True)
        readout = numer_v[h] / jnp.maximum(jnp.abs(denom), floor[:, h : h + 1])
        energy = energy + jnp.sum(readout * readout, axis=-1, keepdims=True)
        gated.append((readout * head_gain_ref[h : h + 1, :] * jax.nn.sigmoid(outgates[h])).astype(jnp.bfloat16))
    loads[4 + CHUNKS].wait()
    part_ref[:, 0:width] = dot32(jnp.concatenate(gated, axis=1), merge_v[...])
    part_ref[:, width : width + LANES] = jnp.broadcast_to(energy, (own_rows, LANES))
    loads = loads[5 + CHUNKS :]
    pl.semaphore_wait(barrier, nep)

    exchange = remote(part_ref, part_in, send_sem.at[0], recv_sem.at[0], partner)
    exchange.start()

    def block_copy(index, device, slot):
        ref = blocks.at[index, :, mine]
        return remote(ref, ref, block_send.at[slot], block_recv.at[index], device)

    if span == 2:
        pair = block_copy(my_block, {"ep": (z + 1 - 2 * zr) * nx + x}, 0)
        pair.start()
    exchange.wait()

    total = part_ref[...] + part_in[...]
    scale = lax.rsqrt(total[:, width : width + 1] / all_width + epsilon)
    resid = (tokens_ref[...].astype(jnp.float32) + scale * total[:, :width]).astype(jnp.bfloat16)
    resid32 = resid.astype(jnp.float32)
    resid_v[...] = resid32
    normed = rms_norm(resid32, gain_ref[...])
    normed_v[...] = normed.astype(jnp.float32)

    experts = lax.broadcasted_iota(jnp.int32, (own_rows, nep), 1)
    picks = [(routes_ref[:, k : k + 1] == experts).astype(jnp.float32) for k in range(2)]
    member = picks[0] + picks[1]
    row_at = lax.broadcasted_iota(jnp.int32, (own_rows, own_rows), 0)
    col_at = lax.broadcasted_iota(jnp.int32, (own_rows, own_rows), 1)
    earlier = (col_at < row_at).astype(jnp.float32)
    rank = dot32(earlier, member)
    chosen = [jnp.where(rank < 0.5, member, 0.0), jnp.where(rank < 0.5, 0.0, member)]

    def to_boxes(values, box):
        for slot in range(2):
            for c in range(pieces):
                relay[pl.ds(slot * pieces + c, nep, stride=2 * pieces), :] = values[slot][
                    :, c * LANES : (c + 1) * LANES
                ]
        box[...] = relay[...].reshape(nep, 2 * pieces, LANES).astype(jnp.bfloat16)

    def from_box(box, slot, c):
        return relay[pl.ds(slot * pieces + c, nep, stride=2 * pieces), :]

    own_half = normed_v[:, mine].astype(jnp.bfloat16)
    to_boxes([dot_tn(chosen[s].astype(jnp.bfloat16), own_half) for s in range(2)], outbox)

    def send_all(src, dst_at, sem):
        @pl.loop(0, nz)
        def _(k):
            away = nz // 2 + (2 * (k % 2) - 1) * ((k + 1) // 2)
            there_z = (z + away) % nz
            for j in range(nx):
                there = there_z * nx + (x + j) % nx

                @pl.when(there != me)
                def _():
                    remote(src.at[there], dst_at, send_sem.at[sem], recv_sem.at[sem], {"ep": there}).start()

    send_all(outbox, inbox.at[t, me], 1)
    inbox[t, me] = outbox[me]

    acts_out[...] = normed_v[pl.ds(pl.multiple_of(t * half_rows, half_rows), half_rows), :].astype(jnp.bfloat16)

    def block_to_x(index, base):
        copies = [block_copy(index, {"ep": z * nx + (x + j) % nx}, base + j) for j in range(1, nx)]
        for copy in copies:
            copy.start()
        return copies

    sent = block_to_x(my_block, 0)

    @pl.loop(1, members)
    def _(i):
        there = ((zi + i) % members) * span + zr
        remote(acts_out, acts.at[zi], send_sem.at[2], recv_sem.at[2], {"ep": there * nx + x}).start()

    acts[zi] = acts_out[...]

    def await_block(index):
        ref = blocks.at[index, :, mine]
        pltpu.make_async_copy(ref, ref, block_recv.at[index]).wait()

    if span == 2:
        other = (1 - zr) * nx + x
        await_block(other)
        sent += block_to_x(other, nx)

    box_bytes = inbox.at[0, pl.ds(0, peers)]
    await_bytes(box_bytes, recv_sem.at[1])
    box_swap = remote(inbox.at[t], inbox.at[t], send_sem.at[3], recv_sem.at[3], partner)
    box_swap.start()
    box_swap.wait_recv()

    for h in range(2):
        relay[...] = inbox[h].astype(jnp.float32).reshape(relay.shape)
        for slot in range(2):
            for c in range(pieces):
                at = h * half + c * LANES
                rows_v[slot * nep : (slot + 1) * nep, at : at + LANES] = from_box(relay, slot, c).astype(jnp.bfloat16)
    loads[0].wait()
    loads[1].wait()
    gate_val = dot32(rows_v[...], gate_v[...])
    up_val = dot32(rows_v[...], up_v[...])
    hidden = (jax.nn.silu(gate_val) * up_val).astype(jnp.bfloat16)
    loads[2].wait()
    for h in range(2):
        half_out[h] = dot32(hidden, down_v[:, h * half : (h + 1) * half]).astype(jnp.bfloat16)
    half_swap = remote(half_out.at[1 - t], half_in, send_sem.at[4], recv_sem.at[4], partner)
    half_swap.start()

    theirs = pl.ds(pl.multiple_of((1 - t) * half, LANES), half)

    def block_swap(index):
        ref = blocks.at[index, :, mine]
        return remote(ref, ref, block_send.at[2 * nx + index], block_recv.at[span * nx + index], partner)

    for i in range(1, span * nx):
        index = (my_block + i) % (span * nx)
        if not (span == 2 and i == nx):
            await_block(index)
        block_swap(index).start()

    half_swap.wait_recv()
    summed = (half_out[t].astype(jnp.float32) + half_in[...].astype(jnp.float32)).astype(jnp.bfloat16)
    summed = summed.astype(jnp.float32)
    await_bytes(box_bytes, send_sem.at[1])
    to_boxes([summed[s * nep : (s + 1) * nep] for s in range(2)], backbox)
    send_all(backbox, homebox.at[me], 5)
    homebox[me] = backbox[me]

    for i in range(1, span * nx):
        index = (my_block + i) % (span * nx)
        ref = blocks.at[index, :, theirs]
        pltpu.make_async_copy(ref, ref, block_recv.at[span * nx + index]).wait()
    act_bytes = acts.at[pl.ds(0, members - 1)]
    await_bytes(act_bytes, recv_sem.at[2])
    dense_rows = acts[...].astype(jnp.float32).reshape(members * half_rows, width).astype(jnp.bfloat16)
    dense = jnp.zeros((members * half_rows, width), jnp.float32)
    for index in range(span * nx):
        left = dot_nt(dense_rows, blocks[index, 0:PADDED, :])
        right = dot_nt(dense_rows, blocks[index, PADDED : 2 * PADDED, :])
        units = (jax.nn.silu(left) * right).astype(jnp.bfloat16)
        dense = dense + dot32(units, blocks[index, 2 * PADDED : 3 * PADDED, :])
    dense_out[...] = dense.reshape(members, half_rows, width).astype(jnp.bfloat16)

    @pl.loop(1, members)
    def _(i):
        mi = (zi + i) % members
        there = mi * span + zr
        remote(dense_out.at[mi], dense_in.at[zi], send_sem.at[6], recv_sem.at[6], {"ep": there * nx + x}).start()

    dense_in[zi] = dense_out[zi]

    scores = scores_ref[...].astype(jnp.float32)
    top = jnp.max(scores, axis=-1, keepdims=True)
    powers = jnp.exp(scores - top)
    weights = powers / jnp.sum(powers, axis=-1, keepdims=True)
    weight_of = weights[:, 0:1] * picks[0] + weights[:, 1:2] * picks[1]
    await_bytes(homebox.at[pl.ds(0, peers)], recv_sem.at[5])
    relay[...] = homebox[...].astype(jnp.float32).reshape(relay.shape)
    routed = []
    for c in range(pieces):
        piece = jnp.zeros((own_rows, LANES), jnp.float32)
        for slot in range(2):
            taken = jnp.where(chosen[slot] > 0.5, weight_of, 0.0)
            piece = piece + dot32(taken, from_box(relay, slot, c), lax.Precision.HIGHEST)
        routed.append(piece)
    routed = jnp.concatenate(routed, axis=1)
    for h in range(2):
        swap_out[h] = routed[h * half_rows : (h + 1) * half_rows]
    swap = remote(swap_out.at[1 - t], swap_in, send_sem.at[7], recv_sem.at[7], partner)
    swap.start()

    home = pl.ds(pl.multiple_of(t * half_rows, half_rows), half_rows)
    own_normed = normed_v[home, :]
    blend = jax.nn.sigmoid(jnp.sum(own_normed * blend_ref[...], axis=-1, keepdims=True))
    await_bytes(dense_in.at[pl.ds(0, members - 1)], recv_sem.at[6])
    base = resid_v[home, :] + blend * jnp.sum(dense_in[...].astype(jnp.float32), axis=0)
    resid_v[home, :] = base
    swap.wait_recv()
    out_ref[:, mine] = (resid_v[home, mine] + swap_out[t]).astype(jnp.bfloat16)
    out_ref[:, theirs] = (resid_v[home, theirs] + swap_in[...]).astype(jnp.bfloat16)

    for store in stores:
        store.wait()
    await_bytes(act_bytes, send_sem.at[2])
    box_swap.wait_send()
    half_swap.wait_send()
    await_bytes(box_bytes, send_sem.at[5])
    await_bytes(dense_in.at[pl.ds(0, members - 1)], send_sem.at[6])
    swap.wait_send()
    if span == 2:
        pair.wait_send()
    for copy in sent:
        copy.wait_send()
    for i in range(1, span * nx):
        block_swap((my_block + i) % (span * nx)).wait_send()


def feed(nep, nx, span, all_width, resident, streamed):
    own_rows, width = resident[0].shape
    half, half_rows = width // 2, own_rows // 2
    pieces = half // LANES
    members = nep // nx // span
    hidden = streamed[6].shape[2]
    here = streamed[0].shape[1]
    matrix = streamed[5]
    bf16, f32 = jnp.bfloat16, jnp.float32
    vmem = pl.BlockSpec(memory_space=pltpu.VMEM)
    hbm = pl.BlockSpec(memory_space=pltpu.HBM)
    box = (nep, 2 * pieces, LANES)
    return pl.pallas_call(
        functools.partial(feed_kernel, nep, nx, span, all_width),
        out_shape=(
            jax.ShapeDtypeStruct((half_rows, width), bf16),
            jax.ShapeDtypeStruct(matrix.shape, f32),
            jax.ShapeDtypeStruct((own_rows, here), f32),
            jax.ShapeDtypeStruct((own_rows, matrix.shape[1]), f32),
        ),
        in_specs=[vmem] * len(resident) + [hbm] * len(streamed),
        out_specs=(vmem, hbm, vmem, vmem),
        scratch_shapes=[
            pltpu.VMEM((4, width, here), bf16),
            pltpu.VMEM((here, width), bf16),
            pltpu.VMEM(matrix.shape, f32),
            pltpu.VMEM((matrix.shape[1], own_rows, matrix.shape[2]), f32),
            pltpu.VMEM((own_rows, width + LANES), f32),
            pltpu.VMEM((width, hidden), bf16),
            pltpu.VMEM((width, hidden), bf16),
            pltpu.VMEM((hidden, width), bf16),
            pltpu.VMEM((own_rows, width + LANES), f32),
            pltpu.VMEM((own_rows, width), f32),
            pltpu.VMEM((own_rows, width), f32),
            pltpu.VMEM((nep * 2 * pieces, LANES), f32),
            pltpu.VMEM(box, bf16),
            pltpu.VMEM((2, *box), bf16),
            pltpu.VMEM((2 * nep, width), bf16),
            pltpu.VMEM((2, 2 * nep, half), bf16),
            pltpu.VMEM((2 * nep, half), bf16),
            pltpu.VMEM(box, bf16),
            pltpu.VMEM(box, bf16),
            pltpu.VMEM((half_rows, width), bf16),
            pltpu.VMEM((members, half_rows, width), bf16),
            pltpu.VMEM((span * nx, 3 * PADDED, width), bf16),
            pltpu.VMEM((members, half_rows, width), bf16),
            pltpu.VMEM((members, half_rows, width), bf16),
            pltpu.VMEM((2, half_rows, half), f32),
            pltpu.VMEM((half_rows, half), f32),
            pltpu.SemaphoreType.DMA((8 + 2 * CHUNKS,)),
            pltpu.SemaphoreType.DMA((8,)),
            pltpu.SemaphoreType.DMA((8,)),
            pltpu.SemaphoreType.DMA((2 * nx + span * nx,)),
            pltpu.SemaphoreType.DMA((2 * span * nx,)),
        ],
        compiler_params=pltpu.CompilerParams(
            collective_id=0, has_side_effects=True, vmem_limit_bytes=60 * 1024 * 1024
        ),
        name="feed",
    )(*resident, *streamed)


def local(
    nx,
    span,
    tokens,
    query_weight,
    key_weight,
    value_weight,
    outgate_weight,
    ingate_weight,
    forget_weight,
    forget_bias,
    head_gain,
    merge_weight,
    mixer_gain,
    feed_gain,
    memory_matrix,
    memory_norm,
    memory_max,
    routes,
    route_scores,
    expert_gate,
    expert_up,
    expert_down,
    dense_left,
    dense_right,
    dense_down,
    blend_weight,
):
    own_rows = tokens.shape[0]

    def padded(rows):
        return jnp.pad(rows, ((0, PADDED - rows.shape[0]), (0, 0)))

    block = jnp.concatenate([padded(dense_left.T), padded(dense_right.T), padded(dense_down)], axis=0)
    resident = (
        tokens,
        routes,
        route_scores,
        mixer_gain[None, :],
        feed_gain[None, :],
        blend_weight[None, :],
        block,
        jnp.concatenate([ingate_weight, forget_weight], axis=1),
        forget_bias[None, :],
        head_gain,
        memory_norm.reshape(own_rows, -1),
        memory_max,
    )
    streamed = (
        query_weight,
        key_weight,
        value_weight,
        outgate_weight,
        merge_weight,
        memory_matrix,
        expert_gate,
        expert_up,
        expert_down,
    )
    all_width = query_weight.shape[1] * lax.axis_size("tp")
    layer_out, matrix, norm, new_max = feed(lax.axis_size("ep"), nx, span, all_width, resident, streamed)
    return (layer_out, matrix, norm.reshape(memory_norm.shape), new_max)


def build(mesh, nx, span):
    return jax.shard_map(
        functools.partial(local, nx, span),
        mesh=mesh,
        in_specs=(
            P(GRP_EP, None),
            P(None, "tp"),
            P(None, "tp"),
            P(None, "tp"),
            P(None, "tp"),
            P(None, "tp"),
            P(None, "tp"),
            P("tp"),
            P("tp", None),
            P("tp", None),
            P(),
            P(),
            P(GRP_EP, "tp", None, None),
            P(GRP_EP, "tp", None),
            P(GRP_EP, "tp"),
            P(GRP_EP, None),
            P(GRP_EP, None),
            P("ep", None, "tp"),
            P("ep", None, "tp"),
            P("ep", "tp", None),
            P(None, "ep"),
            P(None, "ep"),
            P("ep", None),
            P(),
        ),
        out_specs=(
            P(GRP_EP_TP, None),
            P(GRP_EP, "tp", None, None),
            P(GRP_EP, "tp", None),
            P(GRP_EP, "tp"),
        ),
        check_vma=False,
    )


def solution(mesh):
    return build(mesh, NX, SPAN)
```

```python
import functools

import jax
import jax.numpy as jnp
from jax import lax
from jax.experimental import pallas as pl
from jax.experimental.pallas import tpu as pltpu
from jax.sharding import PartitionSpec as P

MESH = pl.DeviceIdType.MESH
GRP_EP = ("grp", "ep")
GRP_EP_TP = ("grp", "ep", "tp")
NX = 4
SPAN = 2
PADDED = 48
CHUNKS = 4
LANES = 128

epsilon = 1e-06


def rms_norm(values, gains):
    floats = values.astype(jnp.float32)
    scaled = floats * lax.rsqrt(jnp.mean(floats * floats, axis=-1, keepdims=True) + epsilon)
    return (scaled * gains).astype(jnp.bfloat16)


def dot32(a, b, precision=None):
    return jnp.dot(a, b, preferred_element_type=jnp.float32, precision=precision)


def dot_nt(a, b):
    return lax.dot_general(a, b, (((1,), (1,)), ((), ())), preferred_element_type=jnp.float32)


def dot_tn(a, b):
    return lax.dot_general(a, b, (((0,), (0,)), ((), ())), preferred_element_type=jnp.float32)


def feed_kernel(
    nep,
    nx,
    span,
    all_width,
    tokens_ref,
    routes_ref,
    scores_ref,
    mixer_ref,
    gain_ref,
    blend_ref,
    left_ref,
    right_ref,
    down_ref,
    ingate_ref,
    forget_ref,
    bias_ref,
    head_gain_ref,
    norm_ref,
    max_ref,
    query_hbm,
    key_hbm,
    value_hbm,
    outgate_hbm,
    merge_hbm,
    matrix_hbm,
    gate_hbm,
    up_hbm,
    down_hbm,
    out_ref,
    matrix_v,
    new_norm_ref,
    new_max_ref,
    project_v,
    merge_v,
    numer_v,
    part_ref,
    gate_v,
    up_v,
    down_v,
    part_in,
    resid_v,
    normed_v,
    relay,
    outbox,
    inbox,
    rows_v,
    half_out,
    half_in,
    backbox,
    homebox,
    acts_out,
    acts,
    blocks,
    dense_out,
    dense_in,
    swap_out,
    swap_in,
    local_sem,
    send_sem,
    recv_sem,
    block_send,
    block_recv,
):
    t = lax.axis_index("tp")
    me = lax.axis_index("ep")
    z, x = me // nx, me % nx
    nz = nep // nx
    members = nz // span
    own_rows, width = tokens_ref.shape
    half = width // 2
    pieces = half // LANES
    half_rows = own_rows // 2
    zi, zr = z // span, z % span
    my_block = zr * nx + x
    peers = nep - 1
    partner = {"tp": 1 - t}

    def remote(src, dst, send, recv, device):
        return pltpu.make_async_remote_copy(
            src_ref=src, dst_ref=dst, send_sem=send, recv_sem=recv, device_id=device, device_id_type=MESH
        )

    def await_bytes(ref, sem):
        pltpu.make_async_copy(ref, ref, sem).wait()

    barrier = pltpu.get_barrier_semaphore()

    @pl.loop(1, nep)
    def _(i):
        pl.semaphore_signal(barrier, inc=1, device_id={"ep": (me + i) % nep}, device_id_type=MESH)

    pl.semaphore_signal(barrier, inc=1, device_id=partner, device_id_type=MESH)
    moves = [(src, project_v.at[i]) for i, src in enumerate((query_hbm, key_hbm, value_hbm, outgate_hbm))]
    chunk = own_rows // CHUNKS
    for c in range(CHUNKS):
        rows = pl.ds(c * chunk, chunk)
        moves.append((matrix_hbm.at[rows], matrix_v.at[rows]))
    moves += [(merge_hbm, merge_v), (gate_hbm.at[0], gate_v), (up_hbm.at[0], up_v), (down_hbm.at[0], down_v)]
    loads = [pltpu.make_async_copy(src, dst, local_sem.at[i]) for i, (src, dst) in enumerate(moves)]
    for load in loads:
        load.start()
    spare = jnp.zeros((PADDED - left_ref.shape[0], width), jnp.bfloat16)
    for i, ref in enumerate((left_ref, right_ref, down_ref)):
        blocks[my_block, i * PADDED : (i + 1) * PADDED, :] = jnp.concatenate([ref[...], spare], axis=0)
    mine = pl.ds(pl.multiple_of(t * half, LANES), half)

    heads, head = head_gain_ref.shape
    row_at = lax.broadcasted_iota(jnp.int32, (own_rows, own_rows), 0)
    col_at = lax.broadcasted_iota(jnp.int32, (own_rows, own_rows), 1)
    same = row_at == col_at

    def upright(rows):
        rows = rows.astype(jnp.float32)
        return [
            jnp.sum(jnp.where(same, rows[i : i + 1, :], 0.0), axis=1, keepdims=True) for i in range(rows.shape[0])
        ]

    first = rms_norm(tokens_ref[...], mixer_ref[...])
    in_gate = dot_nt(first, ingate_ref[...])
    log_forget = jax.nn.log_sigmoid(dot_nt(first, forget_ref[...]) + bias_ref[...])
    old_max = jnp.concatenate(upright(max_ref[...]), axis=1)
    new_max = jnp.maximum(log_forget + old_max, in_gate)
    for h in range(heads):
        new_max_ref[h : h + 1, :] = jnp.sum(jnp.where(same, new_max[:, h : h + 1], 0.0), axis=0, keepdims=True)
    keep = jnp.exp(log_forget + old_max - new_max)
    write = jnp.exp(in_gate - new_max)
    floor = jnp.exp(-new_max)
    projected = []
    for i in range(4):
        loads[i].wait()
        projected.append(dot32(first, project_v[i]))
    by_head = [[p[:, h * head : (h + 1) * head] for h in range(heads)] for p in projected]
    queries, keys, values, outgates = by_head
    written = [write[:, h : h + 1] * (keys[h] * head ** (-0.5)) for h in range(heads)]
    columns = jnp.concatenate(queries + written, axis=0).T
    norms = []
    for h in range(heads):
        norm = keep[:, h : h + 1] * norm_ref[:, h, :] + written[h]
        new_norm_ref[:, h, :] = norm
        norms.append(norm)
    for b in range(own_rows):
        if b % chunk == 0:
            loads[4 + b // chunk].wait()
        for h in range(heads):
            at = h * own_rows + b
            to = heads * own_rows + at
            fresh = keep[b : b + 1, h : h + 1] * matrix_v[b, h] + columns[:, to : to + 1] * values[h][b : b + 1, :]
            matrix_v[b, h] = fresh
            numer_v[h, b : b + 1, :] = jnp.sum(columns[:, at : at + 1] * fresh, axis=0, keepdims=True)
    energy = jnp.zeros((own_rows, 1), jnp.float32)
    gated = []
    for h in range(heads):
        denom = jnp.sum(queries[h] * norms[h], axis=-1, keepdims=True)
        readout = numer_v[h] / jnp.maximum(jnp.abs(denom), floor[:, h : h + 1])
        energy = energy + jnp.sum(readout * readout, axis=-1, keepdims=True)
        gated.append((readout * head_gain_ref[h : h + 1, :] * jax.nn.sigmoid(outgates[h])).astype(jnp.bfloat16))
    loads[4 + CHUNKS].wait()
    part_ref[:, 0:width] = dot32(jnp.concatenate(gated, axis=1), merge_v[...])
    part_ref[:, width : width + LANES] = jnp.broadcast_to(energy, (own_rows, LANES))
    loads = loads[5 + CHUNKS :]
    pl.semaphore_wait(barrier, nep)

    exchange = remote(part_ref, part_in, send_sem.at[0], recv_sem.at[0], partner)
    exchange.start()

    def block_copy(index, device, slot):
        ref = blocks.at[index, :, mine]
        return remote(ref, ref, block_send.at[slot], block_recv.at[index], device)

    if span == 2:
        pair = block_copy(my_block, {"ep": (z + 1 - 2 * zr) * nx + x}, 0)
        pair.start()
    exchange.wait()

    total = part_ref[...] + part_in[...]
    scale = lax.rsqrt(total[:, width : width + 1] / all_width + epsilon)
    resid = (tokens_ref[...].astype(jnp.float32) + scale * total[:, :width]).astype(jnp.bfloat16)
    resid32 = resid.astype(jnp.float32)
    resid_v[...] = resid32
    normed = rms_norm(resid32, gain_ref[...])
    normed_v[...] = normed.astype(jnp.float32)

    experts = lax.broadcasted_iota(jnp.int32, (own_rows, nep), 1).astype(jnp.float32)
    picks = [(named == experts).astype(jnp.float32) for named in upright(routes_ref[...])]
    member = picks[0] + picks[1]
    earlier = (col_at < row_at).astype(jnp.float32)
    rank = dot32(earlier, member)
    chosen = [jnp.where(rank < 0.5, member, 0.0), jnp.where(rank < 0.5, 0.0, member)]

    def to_boxes(values, box):
        for slot in range(2):
            for c in range(pieces):
                relay[pl.ds(slot * pieces + c, nep, stride=2 * pieces), :] = values[slot][
                    :, c * LANES : (c + 1) * LANES
                ]
        box[...] = relay[...].reshape(nep, 2 * pieces, LANES).astype(jnp.bfloat16)

    def from_box(box, slot, c):
        return relay[pl.ds(slot * pieces + c, nep, stride=2 * pieces), :]

    own_half = normed_v[:, mine].astype(jnp.bfloat16)
    to_boxes([dot_tn(chosen[s].astype(jnp.bfloat16), own_half) for s in range(2)], outbox)

    def send_all(src, dst_at, sem):
        @pl.loop(0, nz)
        def _(k):
            away = nz // 2 + (2 * (k % 2) - 1) * ((k + 1) // 2)
            there_z = (z + away) % nz
            for j in range(nx):
                there = there_z * nx + (x + j) % nx

                @pl.when(there != me)
                def _():
                    remote(src.at[there], dst_at, send_sem.at[sem], recv_sem.at[sem], {"ep": there}).start()

    send_all(outbox, inbox.at[t, me], 1)
    inbox[t, me] = outbox[me]

    acts_out[...] = normed_v[pl.ds(pl.multiple_of(t * half_rows, half_rows), half_rows), :].astype(jnp.bfloat16)

    def block_to_x(index, base):
        copies = [block_copy(index, {"ep": z * nx + (x + j) % nx}, base + j) for j in range(1, nx)]
        for copy in copies:
            copy.start()
        return copies

    sent = block_to_x(my_block, 0)

    @pl.loop(1, members)
    def _(i):
        there = ((zi + i) % members) * span + zr
        remote(acts_out, acts.at[zi], send_sem.at[2], recv_sem.at[2], {"ep": there * nx + x}).start()

    acts[zi] = acts_out[...]

    def await_block(index):
        ref = blocks.at[index, :, mine]
        pltpu.make_async_copy(ref, ref, block_recv.at[index]).wait()

    if span == 2:
        other = (1 - zr) * nx + x
        await_block(other)
        sent += block_to_x(other, nx)

    box_bytes = inbox.at[0, pl.ds(0, peers)]
    await_bytes(box_bytes, recv_sem.at[1])
    box_swap = remote(inbox.at[t], inbox.at[t], send_sem.at[3], recv_sem.at[3], partner)
    box_swap.start()
    box_swap.wait_recv()

    for h in range(2):
        relay[...] = inbox[h].astype(jnp.float32).reshape(relay.shape)
        for slot in range(2):
            for c in range(pieces):
                at = h * half + c * LANES
                rows_v[slot * nep : (slot + 1) * nep, at : at + LANES] = from_box(relay, slot, c).astype(jnp.bfloat16)
    loads[0].wait()
    loads[1].wait()
    gate_val = dot32(rows_v[...], gate_v[...])
    up_val = dot32(rows_v[...], up_v[...])
    hidden = (jax.nn.silu(gate_val) * up_val).astype(jnp.bfloat16)
    loads[2].wait()
    for h in range(2):
        half_out[h] = dot32(hidden, down_v[:, h * half : (h + 1) * half]).astype(jnp.bfloat16)
    half_swap = remote(half_out.at[1 - t], half_in, send_sem.at[4], recv_sem.at[4], partner)
    half_swap.start()

    theirs = pl.ds(pl.multiple_of((1 - t) * half, LANES), half)

    def block_swap(index):
        ref = blocks.at[index, :, mine]
        return remote(ref, ref, block_send.at[2 * nx + index], block_recv.at[span * nx + index], partner)

    for i in range(1, span * nx):
        index = (my_block + i) % (span * nx)
        if not (span == 2 and i == nx):
            await_block(index)
        block_swap(index).start()

    half_swap.wait_recv()
    summed = (half_out[t].astype(jnp.float32) + half_in[...].astype(jnp.float32)).astype(jnp.bfloat16)
    summed = summed.astype(jnp.float32)
    await_bytes(box_bytes, send_sem.at[1])
    to_boxes([summed[s * nep : (s + 1) * nep] for s in range(2)], backbox)
    send_all(backbox, homebox.at[me], 5)
    homebox[me] = backbox[me]

    for i in range(1, span * nx):
        index = (my_block + i) % (span * nx)
        ref = blocks.at[index, :, theirs]
        pltpu.make_async_copy(ref, ref, block_recv.at[span * nx + index]).wait()
    act_bytes = acts.at[pl.ds(0, members - 1)]
    await_bytes(act_bytes, recv_sem.at[2])
    dense_rows = acts[...].astype(jnp.float32).reshape(members * half_rows, width).astype(jnp.bfloat16)
    dense = jnp.zeros((members * half_rows, width), jnp.float32)
    for index in range(span * nx):
        left = dot_nt(dense_rows, blocks[index, 0:PADDED, :])
        right = dot_nt(dense_rows, blocks[index, PADDED : 2 * PADDED, :])
        units = (jax.nn.silu(left) * right).astype(jnp.bfloat16)
        dense = dense + dot32(units, blocks[index, 2 * PADDED : 3 * PADDED, :])
    dense_out[...] = dense.reshape(members, half_rows, width).astype(jnp.bfloat16)

    @pl.loop(1, members)
    def _(i):
        mi = (zi + i) % members
        there = mi * span + zr
        remote(dense_out.at[mi], dense_in.at[zi], send_sem.at[6], recv_sem.at[6], {"ep": there * nx + x}).start()

    dense_in[zi] = dense_out[zi]

    scores = upright(scores_ref[...])
    top = jnp.maximum(scores[0], scores[1])
    powers = [jnp.exp(score - top) for score in scores]
    weight_of = (powers[0] * picks[0] + powers[1] * picks[1]) / (powers[0] + powers[1])
    await_bytes(homebox.at[pl.ds(0, peers)], recv_sem.at[5])
    relay[...] = homebox[...].astype(jnp.float32).reshape(relay.shape)
    routed = []
    for c in range(pieces):
        piece = jnp.zeros((own_rows, LANES), jnp.float32)
        for slot in range(2):
            taken = jnp.where(chosen[slot] > 0.5, weight_of, 0.0)
            piece = piece + dot32(taken, from_box(relay, slot, c), lax.Precision.HIGHEST)
        routed.append(piece)
    routed = jnp.concatenate(routed, axis=1)
    for h in range(2):
        swap_out[h] = routed[h * half_rows : (h + 1) * half_rows]
    swap = remote(swap_out.at[1 - t], swap_in, send_sem.at[7], recv_sem.at[7], partner)
    swap.start()

    home = pl.ds(pl.multiple_of(t * half_rows, half_rows), half_rows)
    own_normed = normed_v[home, :]
    blend = jax.nn.sigmoid(jnp.sum(own_normed * blend_ref[...], axis=-1, keepdims=True))
    await_bytes(dense_in.at[pl.ds(0, members - 1)], recv_sem.at[6])
    base = resid_v[home, :] + blend * jnp.sum(dense_in[...].astype(jnp.float32), axis=0)
    resid_v[home, :] = base
    swap.wait_recv()
    out_ref[:, mine] = (resid_v[home, mine] + swap_out[t]).astype(jnp.bfloat16)
    out_ref[:, theirs] = (resid_v[home, theirs] + swap_in[...]).astype(jnp.bfloat16)

    await_bytes(act_bytes, send_sem.at[2])
    box_swap.wait_send()
    half_swap.wait_send()
    await_bytes(box_bytes, send_sem.at[5])
    await_bytes(dense_in.at[pl.ds(0, members - 1)], send_sem.at[6])
    swap.wait_send()
    if span == 2:
        pair.wait_send()
    for copy in sent:
        copy.wait_send()
    for i in range(1, span * nx):
        block_swap((my_block + i) % (span * nx)).wait_send()


def feed(nep, nx, span, all_width, resident, streamed):
    own_rows, width = resident[0].shape
    half, half_rows = width // 2, own_rows // 2
    pieces = half // LANES
    members = nep // nx // span
    hidden = streamed[6].shape[2]
    here = streamed[0].shape[1]
    matrix = streamed[5]
    bf16, f32 = jnp.bfloat16, jnp.float32
    vmem = pl.BlockSpec(memory_space=pltpu.VMEM)
    hbm = pl.BlockSpec(memory_space=pltpu.HBM)
    box = (nep, 2 * pieces, LANES)
    return pl.pallas_call(
        functools.partial(feed_kernel, nep, nx, span, all_width),
        out_shape=(
            pltpu.VMEM((half_rows, width), bf16),
            pltpu.VMEM(matrix.shape, f32),
            pltpu.VMEM((own_rows, *matrix.shape[1:3]), f32),
            pltpu.VMEM((matrix.shape[1], own_rows), f32),
        ),
        in_specs=[vmem] * len(resident) + [hbm] * len(streamed),
        out_specs=(vmem, vmem, vmem, vmem),
        scratch_shapes=[
            pltpu.VMEM((4, width, here), bf16),
            pltpu.VMEM((here, width), bf16),
            pltpu.VMEM((matrix.shape[1], own_rows, matrix.shape[2]), f32),
            pltpu.VMEM((own_rows, width + LANES), f32),
            pltpu.VMEM((width, hidden), bf16),
            pltpu.VMEM((width, hidden), bf16),
            pltpu.VMEM((hidden, width), bf16),
            pltpu.VMEM((own_rows, width + LANES), f32),
            pltpu.VMEM((own_rows, width), f32),
            pltpu.VMEM((own_rows, width), f32),
            pltpu.VMEM((nep * 2 * pieces, LANES), f32),
            pltpu.VMEM(box, bf16),
            pltpu.VMEM((2, *box), bf16),
            pltpu.VMEM((2 * nep, width), bf16),
            pltpu.VMEM((2, 2 * nep, half), bf16),
            pltpu.VMEM((2 * nep, half), bf16),
            pltpu.VMEM(box, bf16),
            pltpu.VMEM(box, bf16),
            pltpu.VMEM((half_rows, width), bf16),
            pltpu.VMEM((members, half_rows, width), bf16),
            pltpu.VMEM((span * nx, 3 * PADDED, width), bf16),
            pltpu.VMEM((members, half_rows, width), bf16),
            pltpu.VMEM((members, half_rows, width), bf16),
            pltpu.VMEM((2, half_rows, half), f32),
            pltpu.VMEM((half_rows, half), f32),
            pltpu.SemaphoreType.DMA((8 + CHUNKS,)),
            pltpu.SemaphoreType.DMA((8,)),
            pltpu.SemaphoreType.DMA((8,)),
            pltpu.SemaphoreType.DMA((2 * nx + span * nx,)),
            pltpu.SemaphoreType.DMA((2 * span * nx,)),
        ],
        compiler_params=pltpu.CompilerParams(
            collective_id=0, has_side_effects=True, vmem_limit_bytes=61 * 1024 * 1024
        ),
        name="feed",
    )(*resident, *streamed)


def finish_kernel(layer_in, matrix_in, norm_in, max_in, layer_out, matrix_out, norm_out, max_out, sem):
    copies = [
        pltpu.make_async_copy(src, dst, sem.at[i])
        for i, (src, dst) in enumerate(
            ((matrix_in, matrix_out), (layer_in, layer_out), (norm_in, norm_out), (max_in, max_out))
        )
    ]
    for copy in copies:
        copy.start()
    for copy in copies:
        copy.wait()


def finish(arrays):
    return pl.pallas_call(
        finish_kernel,
        out_shape=tuple(jax.ShapeDtypeStruct(a.shape, a.dtype) for a in arrays),
        in_specs=[pl.BlockSpec(memory_space=pltpu.VMEM)] * len(arrays),
        out_specs=tuple([pl.BlockSpec(memory_space=pltpu.HBM)] * len(arrays)),
        scratch_shapes=[pltpu.SemaphoreType.DMA((len(arrays),))],
        compiler_params=pltpu.CompilerParams(vmem_limit_bytes=16 * 1024 * 1024),
        name="finish",
    )(*arrays)


def local(
    nx,
    span,
    tokens,
    query_weight,
    key_weight,
    value_weight,
    outgate_weight,
    ingate_weight,
    forget_weight,
    forget_bias,
    head_gain,
    merge_weight,
    mixer_gain,
    feed_gain,
    memory_matrix,
    memory_norm,
    memory_max,
    routes,
    route_scores,
    expert_gate,
    expert_up,
    expert_down,
    dense_left,
    dense_right,
    dense_down,
    blend_weight,
):
    resident = (
        tokens,
        routes.T,
        route_scores.T,
        mixer_gain[None, :],
        feed_gain[None, :],
        blend_weight[None, :],
        dense_left.T,
        dense_right.T,
        dense_down,
        ingate_weight.T,
        forget_weight.T,
        forget_bias[None, :],
        head_gain,
        memory_norm,
        memory_max.T,
    )
    streamed = (
        query_weight,
        key_weight,
        value_weight,
        outgate_weight,
        merge_weight,
        memory_matrix,
        expert_gate,
        expert_up,
        expert_down,
    )
    all_width = query_weight.shape[1] * lax.axis_size("tp")
    results = feed(lax.axis_size("ep"), nx, span, all_width, resident, streamed)
    layer_out, matrix, norm, new_max = finish(results)
    return (layer_out, matrix, norm, new_max.T)


def build(mesh, nx, span):
    return jax.shard_map(
        functools.partial(local, nx, span),
        mesh=mesh,
        in_specs=(
            P(GRP_EP, None),
            P(None, "tp"),
            P(None, "tp"),
            P(None, "tp"),
            P(None, "tp"),
            P(None, "tp"),
            P(None, "tp"),
            P("tp"),
            P("tp", None),
            P("tp", None),
            P(),
            P(),
            P(GRP_EP, "tp", None, None),
            P(GRP_EP, "tp", None),
            P(GRP_EP, "tp"),
            P(GRP_EP, None),
            P(GRP_EP, None),
            P("ep", None, "tp"),
            P("ep", None, "tp"),
            P("ep", "tp", None),
            P(None, "ep"),
            P(None, "ep"),
            P("ep", None),
            P(),
        ),
        out_specs=(
            P(GRP_EP_TP, None),
            P(GRP_EP, "tp", None, None),
            P(GRP_EP, "tp", None),
            P(GRP_EP, "tp"),
        ),
        check_vma=False,
    )


def solution(mesh):
    return build(mesh, NX, SPAN)
```
